32 devices in a mesh: grp: 2 (over y), ep: 4 (over z), tp: 4 (over x, core).
Axes of the slice: x: 2, y: 2, z: 4, core: 2. Of those that a mesh axis runs over, the one named last changes fastest.
Arguments:
- out_gate: bfloat16 [1536, 4096], P(('grp', 'ep'), 'tp'), parts along dimension 0, may hold values from -6 to 6
- in_gate: bfloat16 [1536, 4096], P(('grp', 'ep'), 'tp'), parts along dimension 0, may hold values from -6 to 6
- values: bfloat16 [1536, 4096], P(('grp', 'ep'), 'tp'), parts along dimension 0, may hold values from -6 to 6
- conv_taps: float32 [3, 4096], P(None, 'tp'), may hold values from -3 to 3
- mixer_weight: bfloat16 [4096, 4096], P(None, 'tp'), may hold values from -0.09375 to 0.09375
- expert_input: bfloat16 [1536, 4096], P(('grp', 'ep', 'tp')), parts along dimension 0, may hold values from -6 to 6
- norm_gain: float32 [4096], replicated, may hold values from 0.1 to 1.9
- route_ids: int32 [1536, 2], P(('grp', 'ep')), parts along dimension 0, may hold values from 0 to 3, all different within a row; in each aligned block of 48 rows (0 to 47, 48 to 95, ...) at most 48 rows name the same one
- route_weights: float32 [1536, 2], P(('grp', 'ep')), parts along dimension 0, may hold values from 0.25 to 1.25
- gate_weight: bfloat16 [4, 4096, 1024], P('ep', None, 'tp'), may hold values from -0.09375 to 0.09375
- up_weight: bfloat16 [4, 4096, 1024], P('ep', None, 'tp'), may hold values from -0.09375 to 0.09375
- down_weight: bfloat16 [4, 1024, 4096], P('ep', None, 'tp'), may hold values from -0.1875 to 0.1875
- shared_gate: bfloat16 [4096, 512], P(None, 'tp'), may hold values from -0.09375 to 0.09375
- shared_up: bfloat16 [4096, 512], P(None, 'tp'), may hold values from -0.09375 to 0.09375
- shared_down: bfloat16 [512, 4096], P(None, 'tp'), may hold values from -0.25 to 0.25
Outputs:
- mixer_output: bfloat16 [1536, 4096], P(('grp', 'ep'), 'tp'), parts along dimension 0
- expert_output: bfloat16 [1536, 4096], P(('grp', 'ep'), 'tp'), parts along dimension 0
The draws below stay inside these ranges and needn't reach their ends.
There are 2 independent parts, one for each index of `grp`. The reference program is written for one: setup_inputs(seed, part) draws one part's arguments, and reference() takes and returns one part's arrays. A program takes and returns all parts, laid end to end along the dimension named above; an argument that names none is the same for every part. Nothing has to cross between parts.
Inputs may be any that keep to these rules, and one draw needn't show every extreme that they name: `route_ids`: the 2 entries of a row differ. In each aligned block of 48 rows (the routed tokens of one device) no expert is named by more than 48 rows, and in some block an expert is named by exactly 48 rows.
All inputs are finite; a program needn't handle non-finite values.
Results may differ from the reference program's by a relative error of at most 0.0067.
Values may be sent and summed in bfloat16 or wider, within the bound.
No kernel may reach another device: no remote copies, remote signals or barrier semaphores. Data moves between devices by JAX's collectives and lax.ppermute only.
A program may use at most 64 MiB of HBM per device.

```python
import math
import jax
import jax.numpy as jnp
import numpy as np
from jax import lax

D = 4096
FF = 1024
SFF = 512
TOP_K = 2
TAPS = 3
TOKENS = 768
EXPERTS = 4
LANE_ROWS = 48
CAP = 48
N_EP = 4
N_TP = 4


def steps_of(key, shape, shards, least, top_value):
    gain, own = 1.0, jax.random.fold_in(key, 6)
    for dim, shards_of in shards:
        heights = jnp.exp(jax.random.uniform(jax.random.fold_in(own, dim), (shards_of,), jnp.float32, least / len(shards), top_value / len(shards)))
        gain = gain * jnp.repeat(heights, shape[dim] // shards_of).reshape([-1 if axis == dim else 1 for axis in range(len(shape))])
    return gain


def assign_block(stream_key, own, number, rows, number_of, top, bound, skew):
    ranking = jax.random.permutation(stream_key, number_of)
    heavy_load, ordinary = shares(number_of, rows * top, bound, skew, True), shares(number_of, rows * top, bound, skew, False)
    places = jnp.arange(number_of)

    def named(lengths, offset_by):
        used = int((lengths > 0).sum())
        fixed = max(1, used // 4)
        moved = fixed + (places - fixed + offset_by * (used - fixed)) % max(1, number_of - fixed)
        return jnp.zeros((number_of,), jnp.int32).at[ranking[jnp.where(places < fixed, places, moved)]].set(jnp.asarray(lengths, jnp.int32))

    lengths = jnp.where(number % 4 == 0, named(heavy_load, number // 4), named(ordinary, number - number // 4 - 1))
    mixed = jax.random.permutation(jax.random.fold_in(own, 3), number_of)
    giver, receiver = mixed[0:number_of // 2 * 2:2], mixed[1:number_of // 2 * 2:2]
    margin = jnp.minimum(lengths[giver] - 1, bound - lengths[receiver]) // 2
    margin = jnp.where((giver == ranking[0]) | (receiver == ranking[0]) | (lengths[receiver] == 0), 0, jnp.maximum(margin, 0))
    moved = jax.random.randint(jax.random.fold_in(own, 4), (number_of // 2,), 0, 1 << 20) % (margin + 1)
    lengths = lengths.at[giver].add(-moved).at[receiver].add(moved)
    labels = jnp.searchsorted(jnp.cumsum(lengths), jnp.arange(rows * top), side="right").astype(jnp.int32)
    listing = labels.reshape(top, rows).T
    listing = listing[jax.random.permutation(jax.random.fold_in(own, 1), rows)]
    offset_by = jax.random.randint(jax.random.fold_in(own, 2), (rows, 1), 0, top)
    return jnp.take_along_axis(listing, (jnp.arange(top)[None, :] + offset_by) % top, axis=1)


def shares(count, total, reach, lean, full):
    weights = [(1 << 20) // math.isqrt(grade ** lean) + 1 for grade in range(1, count + 1)]
    largest = reach if full else min(reach, max(-(-total // count), total * weights[0] // sum(weights)))
    least = 1 if total - largest >= count - 1 else 0
    counts, spare = [largest] + [least] * (count - 1), total - largest - least * (count - 1)
    while spare > 0:
        movable = [i for i in range(1, count) if counts[i] < largest] or [i for i in range(1, count) if counts[i] < reach]
        whole, budget = sum([weights[i] for i in movable]), spare
        for i in movable:
            extra = min(reach - counts[i], max(1, budget * weights[i] // whole), spare)
            counts[i] = counts[i] + extra
            spare = spare - extra
    return np.array(counts)


def bell_draw(key, extent, deviation, most, pieces=(), kind=jnp.bfloat16):
    values = deviation * jax.random.normal(key, extent, jnp.float32)
    if pieces:
        values = values * steps_of(key, extent, pieces, -0.22, 0.18)
    return jnp.clip(values, -most, most).astype(kind)


def setup_inputs(seed: int = 0, part: int = 0) -> dict:
    seeds = jax.random.split(jax.random.key(seed), 16)
    part_keys = jax.random.split(jax.random.fold_in(seeds[15], part), 16)
    out_gate = bell_draw(part_keys[0], (TOKENS, D), 1.0, 6.0, ((0, 4), (1, 4)))
    in_gate = bell_draw(part_keys[1], (TOKENS, D), 1.0, 6.0, ((0, 4), (1, 4)))
    values = bell_draw(part_keys[2], (TOKENS, D), 1.0, 6.0, ((0, 4), (1, 4)))
    conv_taps = bell_draw(seeds[3], (TAPS, D), 0.6, 3.0, ((1, 4),), jnp.float32)
    mixer_weight = bell_draw(seeds[4], (D, D), D ** -0.5, 0.09375, ((1, 4),))
    expert_input = bell_draw(part_keys[5], (TOKENS, D), 1.0, 6.0, ((0, 16),))
    norm_gain = jnp.clip(1.0 + 0.18 * jax.random.normal(seeds[6], (D,), jnp.float32), 0.1, 1.9)
    route_ids_keys = jax.random.split(jax.random.fold_in(part_keys[7], 1), TOKENS // LANE_ROWS)
    route_ids_turns = jax.random.permutation(jax.random.fold_in(part_keys[7], 3), TOKENS // LANE_ROWS)
    route_ids = jax.vmap(lambda own, number: assign_block(jax.random.fold_in(part_keys[7], 2), own, number, LANE_ROWS, EXPERTS, TOP_K, CAP, 2))(route_ids_keys, route_ids_turns).reshape((TOKENS, TOP_K))
    route_weights = jnp.clip(0.25 + 1.0 * jax.random.uniform(part_keys[8], (TOKENS, TOP_K), jnp.float32) ** steps_of(part_keys[8], (TOKENS, TOP_K), ((0, 4),), -0.2, 0.2), 0.25, 1.25)
    gate_weight = bell_draw(seeds[9], (EXPERTS, D, FF), D ** -0.5, 0.09375, ((0, 4), (2, 4)))
    up_weight = bell_draw(seeds[10], (EXPERTS, D, FF), D ** -0.5, 0.09375, ((0, 4), (2, 4)))
    down_weight = bell_draw(seeds[11], (EXPERTS, FF, D), FF ** -0.5, 0.1875, ((0, 4), (2, 4)))
    shared_gate = bell_draw(seeds[12], (D, SFF), D ** -0.5, 0.09375, ((1, 4),))
    shared_up = bell_draw(seeds[13], (D, SFF), D ** -0.5, 0.09375, ((1, 4),))
    shared_down = bell_draw(seeds[14], (SFF, D), SFF ** -0.5, 0.25, ((1, 4),))
    return dict(out_gate=out_gate, in_gate=in_gate, values=values, conv_taps=conv_taps, mixer_weight=mixer_weight, expert_input=expert_input, norm_gain=norm_gain, route_ids=route_ids, route_weights=route_weights, gate_weight=gate_weight, up_weight=up_weight, down_weight=down_weight, shared_gate=shared_gate, shared_up=shared_up, shared_down=shared_down)


norm_floor = 0.5

def layer_norm(tokens, norm_gain):
    widened = tokens.astype(jnp.float32)
    centred = widened - lax.optimization_barrier(jnp.mean(widened, axis=-1, keepdims=True))
    spread = lax.optimization_barrier(jnp.mean(centred * centred, axis=-1, keepdims=True))
    return (centred * lax.rsqrt(spread + norm_floor) * norm_gain).astype(jnp.bfloat16)

def expert_hidden(inputs, gate_part, up_part):
    gate_value = jnp.dot(inputs, gate_part, preferred_element_type=jnp.float32)
    up_value = jnp.dot(inputs, up_part, preferred_element_type=jnp.float32)
    return (jax.nn.silu(gate_value) * up_value).astype(jnp.bfloat16)

def reference(out_gate, in_gate, values, conv_taps, mixer_weight, expert_input, norm_gain, route_ids, route_weights, gate_weight, up_weight, down_weight, shared_gate, shared_up, shared_down):
    gated_values = (in_gate.astype(jnp.float32) * values.astype(jnp.float32)).astype(jnp.bfloat16)
    extended = jnp.concatenate([jnp.zeros((TAPS - 1, D), jnp.bfloat16), gated_values], axis=0).astype(jnp.float32)
    conv_state = conv_taps[0] * extended[:-2] + conv_taps[1] * extended[1:-1] + conv_taps[2] * extended[2:]
    mixed_rows = (out_gate.astype(jnp.float32) * conv_state).astype(jnp.bfloat16)
    mixer_output = jnp.dot(mixed_rows, mixer_weight, preferred_element_type=jnp.float32).astype(jnp.bfloat16)
    normed_rows = layer_norm(expert_input, norm_gain)
    buffer_len = N_EP * N_TP * CAP
    flat_ids = route_ids.reshape(-1).astype(jnp.int32)
    onehot = (flat_ids[:, None] == jnp.arange(EXPERTS, dtype=jnp.int32)[None, :]).astype(jnp.int32)
    slot_index = lax.optimization_barrier(jnp.sum((jnp.cumsum(onehot, axis=0) - onehot) * onehot, axis=1)).astype(jnp.int32)
    positions = flat_ids * buffer_len + slot_index
    owners = jnp.full((EXPERTS * buffer_len,), TOKENS, jnp.int32)
    owners = owners.at[positions].set(jnp.arange(TOKENS * TOP_K, dtype=jnp.int32) // TOP_K)

    def run_expert(operands):
        owner_rows, gate_part, up_part, down_part = operands
        picked = jnp.take(normed_rows, owner_rows, axis=0, mode='fill', fill_value=0)
        hidden = expert_hidden(picked, gate_part, up_part)
        return jnp.dot(hidden, down_part, preferred_element_type=jnp.float32).astype(jnp.bfloat16)
    results = lax.map(run_expert, (owners.reshape(EXPERTS, buffer_len), gate_weight, up_weight, down_weight))
    picked = jnp.take(results.reshape(EXPERTS * buffer_len, D), positions, axis=0).astype(jnp.float32)
    picked = picked.reshape(TOKENS, TOP_K, D)
    shared_hidden = expert_hidden(normed_rows, shared_gate, shared_up)
    shared_result = jnp.dot(shared_hidden, shared_down, preferred_element_type=jnp.float32)
    expert_output = (shared_result + lax.optimization_barrier(jnp.sum(route_weights[:, :, None] * picked, axis=1))).astype(jnp.bfloat16)
    return (mixer_output, expert_output)
```

```python
import jax
import jax.numpy as jnp
from jax import lax
from jax.sharding import PartitionSpec as P

norm_floor = 0.5


def shifted(value, axis, steps):
    count = lax.axis_size(axis)
    leading, last = (max(0, -steps), min(count, count - steps))
    return lax.ppermute(value, axis, [(source, source + steps) for source in range(leading, last)])


def layer_norm(tokens, norm_gain):
    widened = tokens.astype(jnp.float32)
    centred = widened - jnp.mean(widened, axis=-1, keepdims=True)
    spread = jnp.mean(centred * centred, axis=-1, keepdims=True)
    return (centred * lax.rsqrt(spread + norm_floor) * norm_gain).astype(jnp.bfloat16)


def expert_hidden(inputs, gate_part, up_part):
    gate_value = jnp.dot(inputs, gate_part, preferred_element_type=jnp.float32)
    up_value = jnp.dot(inputs, up_part, preferred_element_type=jnp.float32)
    return (jax.nn.silu(gate_value) * up_value).astype(jnp.bfloat16)


def slot_ranks(route_ids, experts, lanes):
    tok_count, top_count = route_ids.shape
    grouped = route_ids.reshape(lanes, tok_count // lanes * top_count)
    onehot = (grouped[:, :, None] == jnp.arange(experts, dtype=jnp.int32)[None, None, :]).astype(
        jnp.int32
    )
    before = jnp.cumsum(onehot, axis=1) - onehot
    return jnp.sum(before * onehot, axis=2).reshape(tok_count, top_count)


def local_routed(
    out_gate,
    in_gate,
    values,
    conv_taps,
    mixer_weight,
    expert_input,
    norm_gain,
    route_ids,
    route_weights,
    gate_weight,
    up_weight,
    down_weight,
    shared_gate,
    shared_up,
    shared_down,
):
    experts = lax.axis_size("ep")
    lanes = lax.axis_size("tp")
    lane_rows = expert_input.shape[0]
    width = expert_input.shape[1]
    tok_count, top_count = route_ids.shape
    capacity = (2 * lane_rows * top_count + experts - 1) // experts
    gated_values = (in_gate.astype(jnp.float32) * values.astype(jnp.float32)).astype(jnp.bfloat16)
    previous = shifted(gated_values[-2:], "ep", 1)
    extended = jnp.concatenate([previous, gated_values], axis=0).astype(jnp.float32)
    conv_state = (
        conv_taps[0] * extended[:-2] + conv_taps[1] * extended[1:-1] + conv_taps[2] * extended[2:]
    )
    mixed_rows = (out_gate.astype(jnp.float32) * conv_state).astype(jnp.bfloat16)
    normed_own = layer_norm(expert_input, norm_gain)
    mixed_whole, normed_rows = (
        lax.all_gather(mixed_rows, "tp", axis=1, tiled=True),
        lax.all_gather(normed_own, "tp", axis=0, tiled=True),
    )
    mixer_output = jnp.dot(mixed_whole, mixer_weight, preferred_element_type=jnp.float32).astype(
        jnp.bfloat16
    )
    shared_part = expert_hidden(normed_rows, shared_gate, shared_up)
    slot_index = slot_ranks(route_ids, experts, lanes)
    lane_of_row = (jnp.arange(tok_count, dtype=jnp.int32) // lane_rows)[:, None]
    positions = (route_ids * lanes + lane_of_row) * capacity + slot_index
    lane_index = lax.axis_index("tp")
    lane_ids = lax.dynamic_slice_in_dim(route_ids, lane_index * lane_rows, lane_rows, 0)
    lane_slots = lax.dynamic_slice_in_dim(slot_index, lane_index * lane_rows, lane_rows, 0)
    lane_places = lane_ids * capacity + lane_slots
    local_rows = jnp.broadcast_to(jnp.arange(lane_rows, dtype=jnp.int32)[:, None], lane_ids.shape)
    owners = jnp.full((experts * capacity,), lane_rows, jnp.int32)
    owners = owners.at[lane_places.reshape(-1)].set(local_rows.reshape(-1))
    outgoing = jnp.take(normed_own, owners, axis=0, mode="fill", fill_value=0)
    arrived = lax.all_to_all(
        outgoing.reshape(experts, capacity, width), "ep", split_axis=0, concat_axis=0, tiled=True
    )
    segment = lax.all_gather(arrived[None], "tp", axis=0, tiled=True)
    hidden_rows = expert_hidden(segment.reshape(-1, width), gate_weight[0], up_weight[0])
    spread_hidden = hidden_rows.reshape(segment.shape[:-1] + (hidden_rows.shape[-1],))
    routed_hidden = jnp.swapaxes(spread_hidden, 0, 1).reshape(-1, spread_hidden.shape[-1])
    routed_whole, shared_whole = (
        lax.all_gather(routed_hidden, "tp", axis=1, tiled=True),
        lax.all_gather(shared_part, "tp", axis=1, tiled=True),
    )
    routed_result = jnp.dot(
        routed_whole, down_weight[0], preferred_element_type=jnp.float32
    ).astype(jnp.bfloat16)
    out_cols = routed_result.shape[-1]
    returned = lax.all_to_all(
        routed_result.reshape(experts, lanes * capacity, out_cols),
        "ep",
        split_axis=0,
        concat_axis=0,
        tiled=True,
    )
    shared_result = jnp.dot(shared_whole, shared_down, preferred_element_type=jnp.float32)
    picked = jnp.take(
        returned.reshape(experts * lanes * capacity, out_cols), positions.reshape(-1), axis=0
    )
    picked = picked.astype(jnp.float32).reshape(tok_count, top_count, out_cols)
    expert_output = (shared_result + jnp.sum(route_weights[:, :, None] * picked, axis=1)).astype(
        jnp.bfloat16
    )
    return (mixer_output, expert_output)


def core_peers(count):
    return [(source, source ^ 1) for source in range(count)]


def order_of_pieces(axis):
    count, own = lax.axis_size(axis), lax.axis_index(axis)
    cols = [(own + 2 * step) % count for step in range(count // 2)]
    return cols + [col + 1 - 2 * (own % 2) for col in cols]


def gather_pieces(value, axis):
    count = lax.axis_size(axis)
    same = [value]
    for step in range(1, count // 2):
        pairs = [((dest + 2 * step) % count, dest) for dest in range(count)]
        same.append(lax.ppermute(value, axis, pairs))
    return same + [lax.ppermute(piece, axis, core_peers(count)) for piece in same]


def rows_in_order(weight, axis):
    size = weight.shape[0] // lax.axis_size(axis)
    return jnp.concatenate(
        [lax.dynamic_slice_in_dim(weight, place * size, size, 0) for place in order_of_pieces(axis)],
        axis=0,
    )


def ring_sum(parts, axis):
    count, own = lax.axis_size(axis), lax.axis_index(axis)
    half = parts.shape[1] // 2
    sums = []
    for sign, low, size in ((1, 0, half), (-1, half, parts.shape[1] - half)):
        pairs = [(source, (source + sign) % count) for source in range(count)]

        def block(offset):
            place = (own - sign * offset) % count
            return lax.dynamic_slice(parts, (place, low, 0), (1, size, parts.shape[2]))[0]

        moving = block(1)
        for step in range(2, count + 1):
            arrived = lax.ppermute(moving, axis, pairs)
            moving = arrived.astype(jnp.float32) + block(step).astype(jnp.float32)
            if step < count:
                moving = moving.astype(jnp.bfloat16)
        sums.append(moving)
    return jnp.concatenate(sums, axis=0)


def local_dense(
    out_gate,
    in_gate,
    values,
    conv_taps,
    mixer_weight,
    expert_input,
    norm_gain,
    route_ids,
    route_weights,
    gate_weight,
    up_weight,
    down_weight,
    shared_gate,
    shared_up,
    shared_down,
):
    experts = lax.axis_size("ep")
    own_block = lax.axis_index("ep")
    tok_count = route_ids.shape[0]
    normed_own = layer_norm(expert_input, norm_gain)
    normed_all = lax.all_gather(normed_own, ("ep", "tp"), axis=0, tiled=True)
    chosen = route_ids[:, :, None] == jnp.arange(experts, dtype=jnp.int32)[None, None, :]
    own_scales = jnp.sum(jnp.where(chosen, route_weights[:, :, None], 0.0), axis=1)
    scales = lax.all_gather(own_scales.T, "ep", axis=1, tiled=True)
    scale = lax.dynamic_slice_in_dim(scales, own_block, 1, 0)[0]
    gated_values = (in_gate.astype(jnp.float32) * values.astype(jnp.float32)).astype(jnp.bfloat16)
    previous = shifted(gated_values[-2:], "ep", 1)
    extended = jnp.concatenate([previous, gated_values], axis=0).astype(jnp.float32)
    conv_state = (
        conv_taps[0] * extended[:-2] + conv_taps[1] * extended[1:-1] + conv_taps[2] * extended[2:]
    )
    mixed_rows = (out_gate.astype(jnp.float32) * conv_state).astype(jnp.bfloat16)
    mixer_rows = rows_in_order(mixer_weight, "tp")
    down_rows = rows_in_order(down_weight[0], "tp")
    shared_rows = rows_in_order(shared_down, "tp")
    mixed_rows, normed_all, mixer_rows, down_rows, shared_rows, scale = lax.optimization_barrier(
        (mixed_rows, normed_all, mixer_rows, down_rows, shared_rows, scale)
    )
    mixed_pieces = gather_pieces(mixed_rows, "tp")
    hidden = expert_hidden(normed_all, gate_weight[0], up_weight[0])
    hidden_pieces = gather_pieces(hidden, "tp")
    normed_rows = lax.dynamic_slice_in_dim(normed_all, own_block * tok_count, tok_count, 0)
    shared_pieces = gather_pieces(expert_hidden(normed_rows, shared_gate, shared_up), "tp")
    mixer_output = jnp.dot(
        jnp.concatenate(mixed_pieces, axis=1), mixer_rows, preferred_element_type=jnp.float32
    ).astype(jnp.bfloat16)
    shared_result = jnp.dot(
        jnp.concatenate(shared_pieces, axis=1), shared_rows, preferred_element_type=jnp.float32
    )
    result = jnp.dot(
        jnp.concatenate(hidden_pieces, axis=1), down_rows, preferred_element_type=jnp.float32
    )
    weighted = (scale[:, None] * result).astype(jnp.bfloat16)
    routed = ring_sum(weighted.reshape(experts, tok_count, -1), "ep")
    expert_output = (shared_result + routed).astype(jnp.bfloat16)
    return (mixer_output, expert_output)


def local(*operands):
    experts, lane_rows, top_count = lax.axis_size("ep"), operands[5].shape[0], operands[7].shape[1]
    dense = 2 * lane_rows * top_count >= experts * lane_rows
    return (local_dense if dense else local_routed)(*operands)


def solution(mesh):
    placed = (
        P(("grp", "ep"), "tp"),
        P(("grp", "ep"), "tp"),
        P(("grp", "ep"), "tp"),
        P(None, "tp"),
        P(None, "tp"),
        P(("grp", "ep", "tp"), None),
        P(),
        P(("grp", "ep"), None),
        P(("grp", "ep"), None),
        P("ep", None, "tp"),
        P("ep", None, "tp"),
        P("ep", None, "tp"),
        P(None, "tp"),
        P(None, "tp"),
        P(None, "tp"),
    )
    return jax.shard_map(
        local,
        mesh=mesh,
        in_specs=placed,
        out_specs=(P(("grp", "ep"), "tp"), P(("grp", "ep"), "tp")),
        check_vma=False,
    )
```

```python
import jax
import jax.numpy as jnp
from jax import lax
from jax.sharding import PartitionSpec as P

norm_floor = 0.5


def shifted(value, axis, steps):
    count = lax.axis_size(axis)
    leading, last = (max(0, -steps), min(count, count - steps))
    return lax.ppermute(value, axis, [(source, source + steps) for source in range(leading, last)])


def layer_norm(tokens, norm_gain):
    widened = tokens.astype(jnp.float32)
    centred = widened - jnp.mean(widened, axis=-1, keepdims=True)
    spread = jnp.mean(centred * centred, axis=-1, keepdims=True)
    return (centred * lax.rsqrt(spread + norm_floor) * norm_gain).astype(jnp.bfloat16)


def expert_hidden(inputs, gate_part, up_part):
    gate_value = jnp.dot(inputs, gate_part, preferred_element_type=jnp.float32)
    up_value = jnp.dot(inputs, up_part, preferred_element_type=jnp.float32)
    return (jax.nn.silu(gate_value) * up_value).astype(jnp.bfloat16)


def slot_ranks(route_ids, experts, lanes):
    tok_count, top_count = route_ids.shape
    grouped = route_ids.reshape(lanes, tok_count // lanes * top_count)
    onehot = (grouped[:, :, None] == jnp.arange(experts, dtype=jnp.int32)[None, None, :]).astype(
        jnp.int32
    )
    before = jnp.cumsum(onehot, axis=1) - onehot
    return jnp.sum(before * onehot, axis=2).reshape(tok_count, top_count)


def local_routed(
    out_gate,
    in_gate,
    values,
    conv_taps,
    mixer_weight,
    expert_input,
    norm_gain,
    route_ids,
    route_weights,
    gate_weight,
    up_weight,
    down_weight,
    shared_gate,
    shared_up,
    shared_down,
):
    experts = lax.axis_size("ep")
    lanes = lax.axis_size("tp")
    lane_rows = expert_input.shape[0]
    width = expert_input.shape[1]
    tok_count, top_count = route_ids.shape
    capacity = (2 * lane_rows * top_count + experts - 1) // experts
    gated_values = (in_gate.astype(jnp.float32) * values.astype(jnp.float32)).astype(jnp.bfloat16)
    previous = shifted(gated_values[-2:], "ep", 1)
    extended = jnp.concatenate([previous, gated_values], axis=0).astype(jnp.float32)
    conv_state = (
        conv_taps[0] * extended[:-2] + conv_taps[1] * extended[1:-1] + conv_taps[2] * extended[2:]
    )
    mixed_rows = (out_gate.astype(jnp.float32) * conv_state).astype(jnp.bfloat16)
    normed_own = layer_norm(expert_input, norm_gain)
    mixed_whole, normed_rows = (
        lax.all_gather(mixed_rows, "tp", axis=1, tiled=True),
        lax.all_gather(normed_own, "tp", axis=0, tiled=True),
    )
    mixer_output = jnp.dot(mixed_whole, mixer_weight, preferred_element_type=jnp.float32).astype(
        jnp.bfloat16
    )
    shared_part = expert_hidden(normed_rows, shared_gate, shared_up)
    slot_index = slot_ranks(route_ids, experts, lanes)
    lane_of_row = (jnp.arange(tok_count, dtype=jnp.int32) // lane_rows)[:, None]
    positions = (route_ids * lanes + lane_of_row) * capacity + slot_index
    lane_index = lax.axis_index("tp")
    lane_ids = lax.dynamic_slice_in_dim(route_ids, lane_index * lane_rows, lane_rows, 0)
    lane_slots = lax.dynamic_slice_in_dim(slot_index, lane_index * lane_rows, lane_rows, 0)
    lane_places = lane_ids * capacity + lane_slots
    local_rows = jnp.broadcast_to(jnp.arange(lane_rows, dtype=jnp.int32)[:, None], lane_ids.shape)
    owners = jnp.full((experts * capacity,), lane_rows, jnp.int32)
    owners = owners.at[lane_places.reshape(-1)].set(local_rows.reshape(-1))
    outgoing = jnp.take(normed_own, owners, axis=0, mode="fill", fill_value=0)
    arrived = lax.all_to_all(
        outgoing.reshape(experts, capacity, width), "ep", split_axis=0, concat_axis=0, tiled=True
    )
    segment = lax.all_gather(arrived[None], "tp", axis=0, tiled=True)
    hidden_rows = expert_hidden(segment.reshape(-1, width), gate_weight[0], up_weight[0])
    spread_hidden = hidden_rows.reshape(segment.shape[:-1] + (hidden_rows.shape[-1],))
    routed_hidden = jnp.swapaxes(spread_hidden, 0, 1).reshape(-1, spread_hidden.shape[-1])
    routed_whole, shared_whole = (
        lax.all_gather(routed_hidden, "tp", axis=1, tiled=True),
        lax.all_gather(shared_part, "tp", axis=1, tiled=True),
    )
    routed_result = jnp.dot(
        routed_whole, down_weight[0], preferred_element_type=jnp.float32
    ).astype(jnp.bfloat16)
    out_cols = routed_result.shape[-1]
    returned = lax.all_to_all(
        routed_result.reshape(experts, lanes * capacity, out_cols),
        "ep",
        split_axis=0,
        concat_axis=0,
        tiled=True,
    )
    shared_result = jnp.dot(shared_whole, shared_down, preferred_element_type=jnp.float32)
    picked = jnp.take(
        returned.reshape(experts * lanes * capacity, out_cols), positions.reshape(-1), axis=0
    )
    picked = picked.astype(jnp.float32).reshape(tok_count, top_count, out_cols)
    expert_output = (shared_result + jnp.sum(route_weights[:, :, None] * picked, axis=1)).astype(
        jnp.bfloat16
    )
    return (mixer_output, expert_output)


def core_peers(count):
    return [(source, source ^ 1) for source in range(count)]


def order_of_pieces(axis):
    count, own = lax.axis_size(axis), lax.axis_index(axis)
    cols = [(own + 2 * step) % count for step in range(count // 2)]
    return cols + [col + 1 - 2 * (own % 2) for col in cols]


def gather_pieces(value, axis):
    count = lax.axis_size(axis)
    same = [value]
    for step in range(1, count // 2):
        pairs = [((dest + 2 * step) % count, dest) for dest in range(count)]
        same.append(lax.ppermute(value, axis, pairs))
    return same + [lax.ppermute(piece, axis, core_peers(count)) for piece in same]


def rows_in_order(weight, axis):
    size = weight.shape[0] // lax.axis_size(axis)
    return jnp.concatenate(
        [lax.dynamic_slice_in_dim(weight, place * size, size, 0) for place in order_of_pieces(axis)],
        axis=0,
    )


def pieces_in_order(pieces, axis):
    count, own = lax.axis_size(axis), lax.axis_index(axis)
    size = pieces.shape[0] // count
    ordered = []
    for place in range(count):
        same = (place - own) % 2 == 0
        base = jnp.where(same, place, place ^ 1)
        rank = ((base - own) % count) // 2 + jnp.where(same, 0, count // 2)
        ordered.append(lax.dynamic_slice_in_dim(pieces, rank * size, size, 0))
    return jnp.concatenate(ordered, axis=0)


def shifted_round(value, axis, steps):
    count = lax.axis_size(axis)
    return lax.ppermute(value, axis, [(place, (place + steps) % count) for place in range(count)])


def local_dense(
    out_gate,
    in_gate,
    values,
    conv_taps,
    mixer_weight,
    expert_input,
    norm_gain,
    route_ids,
    route_weights,
    gate_weight,
    up_weight,
    down_weight,
    shared_gate,
    shared_up,
    shared_down,
):
    experts, lanes = lax.axis_size("ep"), lax.axis_size("tp")
    own_block = lax.axis_index("ep")
    lane_rows = expert_input.shape[0]
    half = lane_rows // 2
    normed_own = layer_norm(expert_input, norm_gain)

    upward, downward, chunks = normed_own[:half], normed_own[half:], [normed_own]
    for step in range(1, experts):
        upward, downward = shifted_round(upward, "ep", 1), shifted_round(downward, "ep", -1)
        chunks.append(jnp.concatenate([upward, downward], axis=0))
    tokens = [jnp.concatenate(gather_pieces(chunk, "tp"), axis=0) for chunk in chunks]

    chosen = route_ids[:, :, None] == jnp.arange(experts, dtype=jnp.int32)[None, None, :]
    own_scales = jnp.sum(jnp.where(chosen, route_weights[:, :, None], 0.0), axis=1).T
    scales = []
    for step in range(experts):
        row = lax.dynamic_slice_in_dim(own_scales, (own_block + step) % experts, 1, 0)
        scales.append(shifted_round(row, "ep", step) if step else row)
    scales = [scale.reshape(lanes, lane_rows, 1) for scale in scales]

    gated_values = (in_gate.astype(jnp.float32) * values.astype(jnp.float32)).astype(jnp.bfloat16)
    previous = shifted(gated_values[-2:], "ep", 1)
    extended = jnp.concatenate([previous, gated_values], axis=0).astype(jnp.float32)
    conv_state = (
        conv_taps[0] * extended[:-2] + conv_taps[1] * extended[1:-1] + conv_taps[2] * extended[2:]
    )
    mixed_rows = (out_gate.astype(jnp.float32) * conv_state).astype(jnp.bfloat16)
    mixer_rows = rows_in_order(mixer_weight, "tp")
    down_rows = rows_in_order(down_weight[0], "tp")
    shared_rows = rows_in_order(shared_down, "tp")
    mixed_rows, tokens[-1], mixer_rows, down_rows, shared_rows = lax.optimization_barrier(
        (mixed_rows, tokens[-1], mixer_rows, down_rows, shared_rows)
    )

    def contributions(step):
        hidden = expert_hidden(tokens[step], gate_weight[0], up_weight[0])
        hidden = pieces_in_order(hidden, "tp")
        result = jnp.dot(
            jnp.concatenate(gather_pieces(hidden, "tp"), axis=1),
            down_rows,
            preferred_element_type=jnp.float32,
        ).reshape(lanes, lane_rows, -1)
        below, above = scales[step], scales[-step % experts]
        return (
            (below[:, :half] * result[:, :half]).astype(jnp.bfloat16),
            (above[:, half:] * result[:, half:]).astype(jnp.bfloat16),
        )

    rising, falling = contributions(1)
    for step in range(2, experts + 1):
        up_part, down_part = contributions(step % experts)
        rising = shifted_round(rising, "ep", 1).astype(jnp.float32) + up_part
        falling = shifted_round(falling, "ep", -1).astype(jnp.float32) + down_part
        if step < experts:
            rising, falling = rising.astype(jnp.bfloat16), falling.astype(jnp.bfloat16)
    routed = jnp.concatenate([rising, falling], axis=1)

    shared_hidden = pieces_in_order(expert_hidden(tokens[0], shared_gate, shared_up), "tp")
    shared_pieces = gather_pieces(shared_hidden, "tp")
    shared_result = jnp.dot(
        jnp.concatenate(shared_pieces, axis=1), shared_rows, preferred_element_type=jnp.float32
    )
    mixed_pieces = gather_pieces(mixed_rows, "tp")
    mixer_output = jnp.dot(
        jnp.concatenate(mixed_pieces, axis=1), mixer_rows, preferred_element_type=jnp.float32
    ).astype(jnp.bfloat16)
    expert_output = shared_result + routed.reshape(shared_result.shape)
    return (mixer_output, expert_output.astype(jnp.bfloat16))


def local(*operands):
    experts, lane_rows, top_count = lax.axis_size("ep"), operands[5].shape[0], operands[7].shape[1]
    dense = 2 * lane_rows * top_count >= experts * lane_rows
    return (local_dense if dense else local_routed)(*operands)


def solution(mesh):
    placed = (
        P(("grp", "ep"), "tp"),
        P(("grp", "ep"), "tp"),
        P(("grp", "ep"), "tp"),
        P(None, "tp"),
        P(None, "tp"),
        P(("grp", "ep", "tp"), None),
        P(),
        P(("grp", "ep"), None),
        P(("grp", "ep"), None),
        P("ep", None, "tp"),
        P("ep", None, "tp"),
        P("ep", None, "tp"),
        P(None, "tp"),
        P(None, "tp"),
        P(None, "tp"),
    )
    return jax.shard_map(
        local,
        mesh=mesh,
        in_specs=placed,
        out_specs=(P(("grp", "ep"), "tp"), P(("grp", "ep"), "tp")),
        check_vma=False,
    )
```

```python
import jax
import jax.numpy as jnp
from jax import lax
from jax.sharding import PartitionSpec as P

norm_floor = 0.5


def shifted(value, axis, steps):
    count = lax.axis_size(axis)
    leading, last = (max(0, -steps), min(count, count - steps))
    return lax.ppermute(value, axis, [(source, source + steps) for source in range(leading, last)])


def layer_norm(tokens, norm_gain):
    widened = tokens.astype(jnp.float32)
    centred = widened - jnp.mean(widened, axis=-1, keepdims=True)
    spread = jnp.mean(centred * centred, axis=-1, keepdims=True)
    return (centred * lax.rsqrt(spread + norm_floor) * norm_gain).astype(jnp.bfloat16)


def expert_hidden(inputs, gate_part, up_part):
    gate_value = jnp.dot(inputs, gate_part, preferred_element_type=jnp.float32)
    up_value = jnp.dot(inputs, up_part, preferred_element_type=jnp.float32)
    return (jax.nn.silu(gate_value) * up_value).astype(jnp.bfloat16)


def slot_ranks(route_ids, experts, lanes):
    tok_count, top_count = route_ids.shape
    grouped = route_ids.reshape(lanes, tok_count // lanes * top_count)
    onehot = (grouped[:, :, None] == jnp.arange(experts, dtype=jnp.int32)[None, None, :]).astype(
        jnp.int32
    )
    before = jnp.cumsum(onehot, axis=1) - onehot
    return jnp.sum(before * onehot, axis=2).reshape(tok_count, top_count)


def local_routed(
    out_gate,
    in_gate,
    values,
    conv_taps,
    mixer_weight,
    expert_input,
    norm_gain,
    route_ids,
    route_weights,
    gate_weight,
    up_weight,
    down_weight,
    shared_gate,
    shared_up,
    shared_down,
):
    experts = lax.axis_size("ep")
    lanes = lax.axis_size("tp")
    lane_rows = expert_input.shape[0]
    width = expert_input.shape[1]
    tok_count, top_count = route_ids.shape
    capacity = (2 * lane_rows * top_count + experts - 1) // experts
    gated_values = (in_gate.astype(jnp.float32) * values.astype(jnp.float32)).astype(jnp.bfloat16)
    previous = shifted(gated_values[-2:], "ep", 1)
    extended = jnp.concatenate([previous, gated_values], axis=0).astype(jnp.float32)
    conv_state = (
        conv_taps[0] * extended[:-2] + conv_taps[1] * extended[1:-1] + conv_taps[2] * extended[2:]
    )
    mixed_rows = (out_gate.astype(jnp.float32) * conv_state).astype(jnp.bfloat16)
    normed_own = layer_norm(expert_input, norm_gain)
    mixed_whole, normed_rows = (
        lax.all_gather(mixed_rows, "tp", axis=1, tiled=True),
        lax.all_gather(normed_own, "tp", axis=0, tiled=True),
    )
    mixer_output = jnp.dot(mixed_whole, mixer_weight, preferred_element_type=jnp.float32).astype(
        jnp.bfloat16
    )
    shared_part = expert_hidden(normed_rows, shared_gate, shared_up)
    slot_index = slot_ranks(route_ids, experts, lanes)
    lane_of_row = (jnp.arange(tok_count, dtype=jnp.int32) // lane_rows)[:, None]
    positions = (route_ids * lanes + lane_of_row) * capacity + slot_index
    lane_index = lax.axis_index("tp")
    lane_ids = lax.dynamic_slice_in_dim(route_ids, lane_index * lane_rows, lane_rows, 0)
    lane_slots = lax.dynamic_slice_in_dim(slot_index, lane_index * lane_rows, lane_rows, 0)
    lane_places = lane_ids * capacity + lane_slots
    local_rows = jnp.broadcast_to(jnp.arange(lane_rows, dtype=jnp.int32)[:, None], lane_ids.shape)
    owners = jnp.full((experts * capacity,), lane_rows, jnp.int32)
    owners = owners.at[lane_places.reshape(-1)].set(local_rows.reshape(-1))
    outgoing = jnp.take(normed_own, owners, axis=0, mode="fill", fill_value=0)
    arrived = lax.all_to_all(
        outgoing.reshape(experts, capacity, width), "ep", split_axis=0, concat_axis=0, tiled=True
    )
    segment = lax.all_gather(arrived[None], "tp", axis=0, tiled=True)
    hidden_rows = expert_hidden(segment.reshape(-1, width), gate_weight[0], up_weight[0])
    spread_hidden = hidden_rows.reshape(segment.shape[:-1] + (hidden_rows.shape[-1],))
    routed_hidden = jnp.swapaxes(spread_hidden, 0, 1).reshape(-1, spread_hidden.shape[-1])
    routed_whole, shared_whole = (
        lax.all_gather(routed_hidden, "tp", axis=1, tiled=True),
        lax.all_gather(shared_part, "tp", axis=1, tiled=True),
    )
    routed_result = jnp.dot(
        routed_whole, down_weight[0], preferred_element_type=jnp.float32
    ).astype(jnp.bfloat16)
    out_cols = routed_result.shape[-1]
    returned = lax.all_to_all(
        routed_result.reshape(experts, lanes * capacity, out_cols),
        "ep",
        split_axis=0,
        concat_axis=0,
        tiled=True,
    )
    shared_result = jnp.dot(shared_whole, shared_down, preferred_element_type=jnp.float32)
    picked = jnp.take(
        returned.reshape(experts * lanes * capacity, out_cols), positions.reshape(-1), axis=0
    )
    picked = picked.astype(jnp.float32).reshape(tok_count, top_count, out_cols)
    expert_output = (shared_result + jnp.sum(route_weights[:, :, None] * picked, axis=1)).astype(
        jnp.bfloat16
    )
    return (mixer_output, expert_output)


def core_peers(count):
    return [(source, source ^ 1) for source in range(count)]


def order_of_pieces(axis):
    count, own = lax.axis_size(axis), lax.axis_index(axis)
    cols = [(own + 2 * step) % count for step in range(count // 2)]
    return cols + [col + 1 - 2 * (own % 2) for col in cols]


def gather_pieces(value, axis):
    count = lax.axis_size(axis)
    same = [value]
    for step in range(1, count // 2):
        pairs = [((dest + 2 * step) % count, dest) for dest in range(count)]
        same.append(lax.ppermute(value, axis, pairs))
    return same + [lax.ppermute(piece, axis, core_peers(count)) for piece in same]


def rows_in_order(weight, axis):
    size = weight.shape[0] // lax.axis_size(axis)
    return jnp.concatenate(
        [lax.dynamic_slice_in_dim(weight, place * size, size, 0) for place in order_of_pieces(axis)],
        axis=0,
    )


def pieces_in_order(pieces, axis, dim=0):
    count, own = lax.axis_size(axis), lax.axis_index(axis)
    size = pieces.shape[dim] // count
    ordered = []
    for place in range(count):
        same = (place - own) % 2 == 0
        base = jnp.where(same, place, place ^ 1)
        rank = ((base - own) % count) // 2 + jnp.where(same, 0, count // 2)
        ordered.append(lax.dynamic_slice_in_dim(pieces, rank * size, size, dim))
    return jnp.concatenate(ordered, axis=dim)


def shifted_round(value, axis, steps):
    count = lax.axis_size(axis)
    return lax.ppermute(value, axis, [(place, (place + steps) % count) for place in range(count)])


def local_dense(
    out_gate,
    in_gate,
    values,
    conv_taps,
    mixer_weight,
    expert_input,
    norm_gain,
    route_ids,
    route_weights,
    gate_weight,
    up_weight,
    down_weight,
    shared_gate,
    shared_up,
    shared_down,
):
    experts, lanes = lax.axis_size("ep"), lax.axis_size("tp")
    own_block = lax.axis_index("ep")
    lane_rows = expert_input.shape[0]
    half = lane_rows // 2
    normed_own = layer_norm(expert_input, norm_gain)

    upward, downward, chunks = normed_own[:half], normed_own[half:], [normed_own]
    for step in range(1, experts):
        upward, downward = shifted_round(upward, "ep", 1), shifted_round(downward, "ep", -1)
        chunks.append(jnp.concatenate([upward, downward], axis=0))
    chosen = route_ids[:, :, None] == jnp.arange(experts, dtype=jnp.int32)[None, None, :]
    own_scales = jnp.sum(jnp.where(chosen, route_weights[:, :, None], 0.0), axis=1).T
    chunks[-1], own_scales, down_weight, shared_down = lax.optimization_barrier(
        (chunks[-1], own_scales, down_weight, shared_down)
    )
    tokens = [jnp.concatenate(gather_pieces(chunk, "tp"), axis=0) for chunk in chunks]

    scales = []
    for step in range(experts):
        row = lax.dynamic_slice_in_dim(own_scales, (own_block + step) % experts, 1, 0)
        scales.append(shifted_round(row, "ep", step) if step else row)
    scales = [scale.reshape(lanes, lane_rows, 1) for scale in scales]

    gated_values = (in_gate.astype(jnp.float32) * values.astype(jnp.float32)).astype(jnp.bfloat16)
    previous = shifted(gated_values[-2:], "ep", 1)
    extended = jnp.concatenate([previous, gated_values], axis=0).astype(jnp.float32)
    conv_state = (
        conv_taps[0] * extended[:-2] + conv_taps[1] * extended[1:-1] + conv_taps[2] * extended[2:]
    )
    mixed_rows = (out_gate.astype(jnp.float32) * conv_state).astype(jnp.bfloat16)
    down_rows = rows_in_order(down_weight[0], "tp")
    shared_rows = rows_in_order(shared_down, "tp")
    mixed_rows, tokens[-1] = lax.optimization_barrier((mixed_rows, tokens[-1]))

    def contributions(step):
        hidden = expert_hidden(tokens[step], gate_weight[0], up_weight[0])
        hidden = pieces_in_order(hidden, "tp")
        result = jnp.dot(
            jnp.concatenate(gather_pieces(hidden, "tp"), axis=1),
            down_rows,
            preferred_element_type=jnp.float32,
        ).reshape(lanes, lane_rows, -1)
        below, above = scales[step], scales[-step % experts]
        return (
            (below[:, :half] * result[:, :half]).astype(jnp.bfloat16),
            (above[:, half:] * result[:, half:]).astype(jnp.bfloat16),
        )

    rising, falling = contributions(1)
    for step in range(2, experts + 1):
        up_part, down_part = contributions(step % experts)
        rising = shifted_round(rising, "ep", 1).astype(jnp.float32) + up_part
        falling = shifted_round(falling, "ep", -1).astype(jnp.float32) + down_part
        if step < experts:
            rising, falling = rising.astype(jnp.bfloat16), falling.astype(jnp.bfloat16)
    routed = jnp.concatenate([rising, falling], axis=1)

    shared_hidden = pieces_in_order(expert_hidden(tokens[0], shared_gate, shared_up), "tp")
    shared_pieces = gather_pieces(shared_hidden, "tp")
    shared_result = jnp.dot(
        jnp.concatenate(shared_pieces, axis=1), shared_rows, preferred_element_type=jnp.float32
    )
    mixed_pieces = gather_pieces(mixed_rows, "tp")
    mixed_whole = pieces_in_order(jnp.concatenate(mixed_pieces, axis=1), "tp", 1)
    mixer_output = jnp.dot(mixed_whole, mixer_weight, preferred_element_type=jnp.float32).astype(
        jnp.bfloat16
    )
    expert_output = shared_result + routed.reshape(shared_result.shape)
    return (mixer_output, expert_output.astype(jnp.bfloat16))


def local(*operands):
    experts, lane_rows, top_count = lax.axis_size("ep"), operands[5].shape[0], operands[7].shape[1]
    dense = 2 * lane_rows * top_count >= experts * lane_rows
    return (local_dense if dense else local_routed)(*operands)


def solution(mesh):
    placed = (
        P(("grp", "ep"), "tp"),
        P(("grp", "ep"), "tp"),
        P(("grp", "ep"), "tp"),
        P(None, "tp"),
        P(None, "tp"),
        P(("grp", "ep", "tp"), None),
        P(),
        P(("grp", "ep"), None),
        P(("grp", "ep"), None),
        P("ep", None, "tp"),
        P("ep", None, "tp"),
        P("ep", None, "tp"),
        P(None, "tp"),
        P(None, "tp"),
        P(None, "tp"),
    )
    return jax.shard_map(
        local,
        mesh=mesh,
        in_specs=placed,
        out_specs=(P(("grp", "ep"), "tp"), P(("grp", "ep"), "tp")),
        check_vma=False,
    )
```
